512 devices in a mesh: kv: 64 (over z, y), tp: 8 (over x, core).
Axes of the slice: x: 4, y: 8, z: 8, core: 2. Of those that a mesh axis runs over, the one named last changes fastest.
Arguments:
- tokens: bfloat16 [8, 8192, 2048], P(None, 'kv'), may hold values from -32 to 32, as said below
- w_query: bfloat16 [2048, 1024], P(None, 'tp'), may hold values from -0.125 to 0.125
- w_key: bfloat16 [2048, 512], P(None, 'tp'), may hold values from -0.125 to 0.125
- w_value: bfloat16 [2048, 512], P(None, 'tp'), may hold values from -0.125 to 0.125
- w_output: bfloat16 [1024, 2048], P(None, 'tp'), may hold values from -3 to 3
- chosen: int32 [8, 64, 32], P(None, 'kv'), may hold values from -1 to 63, as said below
- lengths: int32 [8], replicated, may hold values from 1 to 8192, 22528 in all
Outputs:
- mixed: bfloat16 [8, 8192, 2048], P(None, 'kv', 'tp')
The draws below stay inside these ranges and needn't reach their ends.
Inputs may be any that keep to these rules, and one draw needn't show every extreme that they name: chosen[s, b] lists distinct blocks of sequence s, none above b; its first entry is b; entries after the named ones are -1. For b >= 1 and each c < b, at most 4 of the 8 lists chosen[:, b] name block c, and exactly 4 of them name block b - 1. lengths[s] is the number of live positions of sequence s; the largest is 8192. `tokens`: activations of order one; some rows may be much larger.
All inputs are finite; a program needn't handle non-finite values.
Results may differ from the reference program's by a relative error of at most 0.012.
The reference program's roundings to bfloat16 on the way count: a program that leaves them out, or rounds other values in their place, can miss the bound.
Values may be sent and summed in bfloat16 or wider, within the bound.
A program may use at most 128 MiB of HBM per device.

```python
import math
import jax
import jax.numpy as jnp
import numpy as np
from jax import lax

D = 2048
HEADS = 16
KV_HEADS = 8
HEAD_DIM = 64
BLK = 128
SEL = 32
SEQS = 8
CAP = 4
SEQ_LEN = 8192
BLOCKS_PER_SEQ = 64


def draw_tokens(key, part):
    shape = (SEQS, SEQ_LEN, D)
    return jnp.clip(jax.random.normal(key, shape, jnp.float32), -6.0, 6.0).astype(jnp.bfloat16)


def draw_chosen(key, part):
    key_allow, key_ordering = jax.random.split(jax.random.fold_in(key, 7))
    owners = jnp.arange(BLOCKS_PER_SEQ, dtype=jnp.int32)
    raw_scores = jax.random.randint(key_allow, (BLOCKS_PER_SEQ, BLOCKS_PER_SEQ, SEQS), 0, 1 << 20) * SEQS + jnp.arange(SEQS, dtype=jnp.int32)
    beaten = jnp.sum((raw_scores[:, :, None, :] > raw_scores[:, :, :, None]).astype(jnp.int32), axis=-1)
    permitted = beaten < CAP
    shard_member = owners[:, None]
    block_keeper = owners[None, :]
    earlier = block_keeper < shard_member
    candidate = earlier[None, :, :] & jnp.transpose(permitted, (2, 0, 1))
    own_block = (block_keeper == shard_member)[None, :, :]
    extra_score = jnp.where(block_keeper == shard_member, 4, jnp.where(block_keeper == shard_member - 1, 3, jnp.where(block_keeper == shard_member - BLOCKS_PER_SEQ // 2, 2, jnp.where(block_keeper == 0, 1, 0))))
    random_jitter = jax.random.randint(key_ordering, (SEQS, BLOCKS_PER_SEQ, BLOCKS_PER_SEQ), 0, 1 << 16)
    block_precedence = (extra_score[None, :, :] * (1 << 20) + random_jitter) * BLOCKS_PER_SEQ + block_keeper[None, :, :]
    block_precedence = jnp.where(candidate | own_block, block_precedence, -1)
    slot_count = min(SEL, BLOCKS_PER_SEQ)
    ranked, _ = lax.top_k(block_precedence, slot_count)
    picked = jnp.where(ranked >= 0, ranked % BLOCKS_PER_SEQ, -1)
    if slot_count < SEL:
        picked = jnp.concatenate([picked, jnp.full((SEQS, BLOCKS_PER_SEQ, SEL - slot_count), -1, jnp.int32)], axis=-1)
    return picked.astype(jnp.int32)


def block_scale(stream_key, dims, shards, smallest, largest):
    factor_of, own = 1.0, jax.random.fold_in(stream_key, 6)
    for axis_at, shards_of in shards:
        draws = jnp.exp(jax.random.uniform(jax.random.fold_in(own, axis_at), (shards_of,), jnp.float32, smallest / len(shards), largest / len(shards)))
        factor_of = factor_of * jnp.repeat(draws, dims[axis_at] // shards_of).reshape([-1 if axis == axis_at else 1 for axis in range(len(dims))])
    return factor_of


def split_up(number_of, total, reach, slope):
    loads = [(1 << 20) // math.isqrt(standing ** slope) + 1 for standing in range(2, number_of + 1)]
    surplus, given = total - reach - (number_of - 1), [1] * (number_of - 1)
    while surplus > 0:
        candidates = [i for i in range(number_of - 1) if given[i] < reach]
        pool, left = sum([loads[i] for i in candidates]), surplus
        for i in candidates:
            addition = min(reach - given[i], max(1, left * loads[i] // pool), surplus)
            given[i] = given[i] + addition
            surplus = surplus - addition
    return np.array([reach] + given)


def ragged(rng, amount, total, limit, skew):
    if amount == 2:
        one = jax.random.randint(rng, (), max(1, total - limit), min(limit, total - 1) + 1)
        return jnp.stack([one, total - one])
    sizes = jnp.asarray(split_up(amount, total, limit, skew), jnp.int32)
    couples = (amount - 1) // 2
    donor, receiver = sizes[1:1 + 2 * couples:2], sizes[2:2 + 2 * couples:2]
    margin = jnp.minimum(donor - 1, limit - receiver)
    shifted = jax.random.randint(jax.random.fold_in(rng, 1), (couples,), 0, 1 << 20) % (margin + 1)
    sizes = sizes.at[1:1 + 2 * couples:2].set(donor - shifted).at[2:2 + 2 * couples:2].set(receiver + shifted)
    return sizes[jax.random.permutation(jax.random.fold_in(rng, 2), amount)]


def bell_draw(key, extent, spread, reach, cuts=(), kind=jnp.bfloat16):
    gain = block_scale(key, extent, cuts, -0.22, 0.18) if cuts else 1.0
    drawn = jax.random.normal(key, extent, jnp.float32) * spread * gain
    return jnp.minimum(jnp.maximum(drawn, -reach), reach).astype(kind)


def setup_inputs(seed: int = 0) -> dict:
    arg_keys = jax.random.split(jax.random.key(seed), 8)
    return {
        "tokens": draw_tokens(jax.random.fold_in(arg_keys[7], 71), 0),
        "w_query": bell_draw(arg_keys[1], (D, HEADS * HEAD_DIM), D ** -0.5, 0.125, ((1, 8),)),
        "w_key": bell_draw(arg_keys[2], (D, KV_HEADS * HEAD_DIM), D ** -0.5, 0.125, ((1, 8),)),
        "w_value": bell_draw(arg_keys[3], (D, KV_HEADS * HEAD_DIM), D ** -0.5, 0.125, ((1, 8),)),
        "w_output": bell_draw(arg_keys[4], (HEADS * HEAD_DIM, D), 0.5, 3.0, ((1, 8),)),
        "chosen": draw_chosen(jax.random.fold_in(arg_keys[7], 71), 0),
        "lengths": ragged(arg_keys[6], SEQS, SEQ_LEN + (SEQS - 1) * SEQ_LEN // 4, SEQ_LEN, 2).astype(jnp.int32),
    }


def attend_block(query_rows, key_seq, value_seq, pick_row, first_pos, length):
    clipped = jnp.maximum(pick_row, 0)
    key_rows = key_seq[clipped].reshape(SEL * BLK, KV_HEADS, HEAD_DIM).astype(jnp.float32)
    value_rows = value_seq[clipped].reshape(SEL * BLK, KV_HEADS, HEAD_DIM).astype(jnp.float32)
    grouped = query_rows.reshape(BLK, KV_HEADS, HEADS // KV_HEADS, HEAD_DIM).astype(jnp.float32)
    scores = jnp.einsum("qkgd,nkd->kgqn", grouped, key_rows) * HEAD_DIM ** -0.5
    query_pos = first_pos + jnp.arange(BLK, dtype=jnp.int32)
    key_pos = (pick_row[:, None] * BLK + jnp.arange(BLK, dtype=jnp.int32)[None, :]).reshape(-1)
    listed = jnp.repeat(pick_row >= 0, BLK)
    allowed = listed[None, :] & (key_pos[None, :] <= query_pos[:, None]) & (key_pos[None, :] < length)
    masked = jnp.where(allowed, scores, -1e30)
    row_max = jnp.max(masked, axis=-1, keepdims=True)
    exponent = jnp.exp(masked - row_max)
    weights = (exponent / jnp.sum(exponent, axis=-1, keepdims=True)).astype(jnp.bfloat16)
    weights = lax.optimization_barrier(weights).astype(jnp.float32)
    mixed_heads = jnp.einsum("kgqn,nkd->qkgd", weights, value_rows)
    live_rows = (query_pos < length)[:, None, None, None]
    return jnp.where(live_rows, mixed_heads, 0.0).astype(jnp.bfloat16).reshape(BLK, HEADS * HEAD_DIM)


def reference(tokens, w_query, w_key, w_value, w_output, chosen, lengths):
    flat_rows = tokens.reshape(SEQS * SEQ_LEN, D)
    queries = lax.optimization_barrier(jnp.dot(flat_rows, w_query, preferred_element_type=jnp.float32).astype(jnp.bfloat16))
    key_proj = lax.optimization_barrier(jnp.dot(flat_rows, w_key, preferred_element_type=jnp.float32).astype(jnp.bfloat16))
    value_proj = lax.optimization_barrier(jnp.dot(flat_rows, w_value, preferred_element_type=jnp.float32).astype(jnp.bfloat16))
    queries = queries.reshape(SEQS, BLOCKS_PER_SEQ, BLK, HEADS * HEAD_DIM)
    key_proj = key_proj.reshape(SEQS, BLOCKS_PER_SEQ, BLK, KV_HEADS, HEAD_DIM)
    value_proj = value_proj.reshape(SEQS, BLOCKS_PER_SEQ, BLK, KV_HEADS, HEAD_DIM)

    def one_seq(packed):
        query_seq, key_seq, value_seq, pick_seq, length = packed

        def one_block(inner_pack):
            query_rows, pick_row, block_id = inner_pack
            return attend_block(query_rows, key_seq, value_seq, pick_row, block_id * BLK, length)

        return lax.map(one_block, (query_seq, pick_seq, jnp.arange(BLOCKS_PER_SEQ, dtype=jnp.int32)))

    attended = lax.map(one_seq, (queries, key_proj, value_proj, chosen, lengths))
    mixed = jnp.dot(attended.reshape(SEQS * SEQ_LEN, HEADS * HEAD_DIM), w_output, preferred_element_type=jnp.float32)
    return mixed.astype(jnp.bfloat16).reshape(SEQS, SEQ_LEN, D)
```

```python
import functools

import jax
import jax.numpy as jnp
from jax import lax
from jax.experimental import pallas as pl
from jax.experimental.pallas import tpu as pltpu
from jax.sharding import PartitionSpec as P

SEQS = 8
BLK = 128
SEL = 32
HD = 64
MESH = pl.DeviceIdType.MESH
LOG2E = 1.4426950408889634
NEG = -1e30
RANKS = (8, 8, 7, 5, 4, 3, 3, 2)
UPTO = (2, 3, 5, 7, 7, 7, 7, 7)


def pick(table, index):
    value = jnp.int32(table[0])
    for i in range(1, len(table)):
        value = jnp.where(index == i, jnp.int32(table[i]), value)
    return value


def project_kernel(
    len_ref, chosen_ref, tok_ref, wq_ref, wk_ref, wv_ref,
    q_ref, kv_ref, bias_ref, meta_ref, tok_buf, w_buf, sems,
):
    block = lax.axis_index("kv")
    first = block * BLK
    for s in range(SEQS):
        rank = jnp.int32(0)
        for t in range(SEQS):
            if t != s:
                ahead = len_ref[t] > len_ref[s] if t > s else len_ref[t] >= len_ref[s]
                rank = rank + ahead.astype(jnp.int32)
        meta_ref[0, rank] = jnp.int32(s)
        meta_ref[1, rank] = len_ref[s]

    def fetch(r):
        return pltpu.make_async_copy(tok_ref.at[meta_ref[0, r]], tok_buf.at[r], sems.at[r])

    for r in range(SEQS):
        fetch(r).start()
    w_buf[:, 0:128] = wq_ref[...]
    w_buf[:, 128:256] = jnp.concatenate([wk_ref[...], wv_ref[...]], axis=1)

    def clear(i, carry):
        bias_ref[i // 64, i % 64] = jnp.float32(NEG)
        return carry

    lax.fori_loop(0, SEQS * 64, clear, 0)

    def mark(i, carry):
        r = i // SEL
        c = chosen_ref[meta_ref[0, r], i % SEL]

        @pl.when(c >= 0)
        def _():
            bias_ref[r, c] = jnp.float32(0.0)

        return carry

    lax.fori_loop(0, SEQS * SEL, mark, 0)
    lane = lax.broadcasted_iota(jnp.int32, (BLK, 128), 1)
    for g in range(SEQS // 2):
        for r in (2 * g, 2 * g + 1):
            fetch(r).wait()
        live = meta_ref[1, 2 * g] > first

        @pl.when(live)
        def _():
            rows = tok_buf[2 * g : 2 * g + 2].reshape(2 * BLK, -1)
            out = jnp.dot(rows, w_buf[...], preferred_element_type=jnp.float32)
            for i in range(2):
                part = out[i * BLK : (i + 1) * BLK]
                q = part[:, 0:128]
                q_ref[2 * g + i, 0:128] = jnp.where(lane < HD, q, 0.0).astype(jnp.bfloat16)
                q_ref[2 * g + i, 128:256] = jnp.where(
                    lane < HD, pltpu.roll(q, HD, 1), 0.0
                ).astype(jnp.bfloat16)
                kv_ref[2 * g + i] = part[:, 128:256].astype(jnp.bfloat16)

        @pl.when(jnp.logical_not(live))
        def _():
            q_ref[2 * g : 2 * g + 2] = jnp.zeros((2, 2 * BLK, 128), jnp.bfloat16)
            kv_ref[2 * g : 2 * g + 2] = jnp.zeros((2, BLK, 128), jnp.bfloat16)


def project(lengths, picked, tokens, w_query, w_key, w_value):
    smem = pl.BlockSpec(memory_space=pltpu.SMEM)
    vmem = pl.BlockSpec(memory_space=pltpu.VMEM)
    return pl.pallas_call(
        project_kernel,
        name="project",
        out_shape=(
            jax.ShapeDtypeStruct((SEQS, 2 * BLK, 128), jnp.bfloat16),
            jax.ShapeDtypeStruct((SEQS, BLK, 128), jnp.bfloat16),
            jax.ShapeDtypeStruct((SEQS, 64), jnp.float32),
            jax.ShapeDtypeStruct((2, SEQS), jnp.int32),
        ),
        in_specs=[smem, smem, pl.BlockSpec(memory_space=pl.ANY), vmem, vmem, vmem],
        out_specs=(vmem, vmem, smem, smem),
        scratch_shapes=[
            pltpu.VMEM((SEQS, BLK, 2048), jnp.bfloat16),
            pltpu.VMEM((2048, 256), jnp.bfloat16),
            pltpu.SemaphoreType.DMA((SEQS,)),
        ],
        compiler_params=pltpu.CompilerParams(vmem_limit_bytes=32 * 1024 * 1024),
    )(lengths, picked, tokens, w_query, w_key, w_value)


def exchange_kernel(
    ranks, bias_ref, meta_ref, q_ref, kv_ref, out_ref,
    buf, att, acc, top, own_sem, recv, send, ring_send, tp_recv, tp_send, out_sem,
):
    sizes = sorted(set(ranks))
    block = lax.axis_index("kv")
    member = lax.axis_index("tp")
    z, y = block // 8, lax.rem(block, 8)
    x, core = member // 2, lax.rem(member, 2)
    mine = pick(ranks, z)

    def at_kv(row, col):
        return {"kv": lax.rem(row + 8, 8) * 8 + lax.rem(col + 8, 8)}

    def at_tp(chip, which):
        return {"tp": lax.rem(chip + 4, 4) * 2 + which}

    own = pltpu.make_async_copy(kv_ref, buf.at[:, block], own_sem)
    own.start()
    barrier = pltpu.get_barrier_semaphore()

    def greet(target):
        pl.semaphore_signal(barrier, inc=1, device_id=target, device_id_type=MESH)

    for target in (
        at_kv(z, y + 1), at_kv(z, y - 1), at_kv(z + 1, y), at_kv(z - 1, y),
        at_tp(x + 1, core), at_tp(x - 1, core), at_tp(x, 1 - core),
    ):
        greet(target)

    @pl.when((z == 1) | (z == 2))
    def _():
        greet(at_kv(jnp.int32(7), y))

    @pl.when(z == 7)
    def _():
        greet(at_kv(jnp.int32(1), y))
        greet(at_kv(jnp.int32(2), y))

    extra = jnp.where((z == 1) | (z == 2), 1, jnp.where(z == 7, 2, 0))
    pl.semaphore_wait(barrier, 7 + extra)
    own.wait()

    def each_size(size, act):
        for k in sizes:
            @pl.when(size == k)
            def _(k=k):
                act(k)

    def link(c, k, sem, target):
        part = buf.at[0:k, c]
        return pltpu.make_async_remote_copy(
            src_ref=part, dst_ref=part, send_sem=sem, recv_sem=recv.at[c],
            device_id=target, device_id_type=MESH,
        )

    def start(c, size, sem, target):
        each_size(size, lambda k: link(c, k, sem, target).start())

    def sent(c, size, sem):
        each_size(size, lambda k: link(c, k, sem, at_kv(z, y + 1)).wait_send())

    def arrived(c, size):
        each_size(size, lambda k: link(c, k, send.at[0, c], at_kv(z, y + 1)).wait_recv())

    def route(row):
        upto = pick(UPTO, row)
        rises = z <= upto
        hops = jnp.where(rises, z - row, 8 - z)
        last_size = pick(ranks, jnp.minimum(upto + 1, 7))
        size_in = jnp.where(rises, mine, last_size)
        up = rises & (z < upto)
        wrap = (z == row) & (upto < 7)
        down = jnp.logical_not(rises) & (z > upto + 1)
        return upto, hops, last_size, size_in, up, wrap, down

    up_size = pick(ranks, jnp.minimum(z + 1, 7))

    def column(act, row, c):
        _, _, last_size, _, up, wrap, down = route(row)

        @pl.when(up)
        def _():
            act(c, up_size, send.at[0, c], at_kv(z + 1, y))

        @pl.when(wrap)
        def _():
            act(c, last_size, send.at[1, c], at_kv(jnp.int32(7), y))

        @pl.when(down)
        def _():
            act(c, last_size, send.at[1, c], at_kv(z - 1, y))

    def left_of(step):
        return lax.rem(y - step + 8, 8)

    def right_of(step):
        return lax.rem(y + step, 8)

    def row_item(act, await_it, row, j):
        step = (j + 1) // 2
        from_left = lax.rem(j, 2) == 1
        c = row * 8 + jnp.where(from_left, left_of(step), right_of(step))
        in_row = row == z
        if await_it:
            _, _, _, size_in, _, _, _ = route(row)

            @pl.when(jnp.logical_not(in_row & (j == 0)))
            def _():
                arrived(c, size_in)

        @pl.when(in_row & ((j == 0) | (from_left & (step < 4))))
        def _():
            act(c, mine, ring_send.at[0, c], at_kv(z, y + 1))

        @pl.when(in_row & (jnp.logical_not(from_left) & (step < 3)))
        def _():
            act(c, mine, ring_send.at[1, c], at_kv(z, y - 1))

        column(act, row, c)

    def column_item(act, await_it, row, step):
        @pl.when(step == 0)
        def _():
            c = row * 8 + y
            if await_it:
                _, _, _, size_in, _, _, _ = route(row)

                @pl.when(row != z)
                def _():
                    arrived(c, size_in)

            act(c, mine, ring_send.at[0, c], at_kv(z, y + 1))
            act(c, mine, ring_send.at[1, c], at_kv(z, y - 1))
            column(act, row, c)

        @pl.when(step > 0)
        def _():
            c = row * 8 + left_of(step)
            if await_it:
                arrived(c, mine)

            @pl.when(step < 4)
            def _():
                act(c, mine, ring_send.at[0, c], at_kv(z, y + 1))

        @pl.when((step > 0) & (step < 4))
        def _():
            c = row * 8 + right_of(step)
            if await_it:
                arrived(c, mine)

            @pl.when(step < 3)
            def _():
                act(c, mine, ring_send.at[1, c], at_kv(z, y - 1))

    def waves(item, items, waves_count):
        def wave(t, carry):
            def one(row, carry):
                _, hops, _, _, _, _, _ = route(row)
                j = t - hops

                @pl.when((j >= 0) & (j < items))
                def _():
                    item(start, True, row, j)

                return carry

            return lax.fori_loop(0, z + 1, one, carry)

        lax.fori_loop(0, waves_count, wave, 0)

    def drain(item, items):
        def one(i, carry):
            item(lambda c, size, sem, target: sent(c, size, sem), False, i // items, lax.rem(i, items))
            return carry

        lax.fori_loop(0, (z + 1) * items, one, 0)

    @pl.when(core == 0)
    def _():
        waves(row_item, 8, 13)

    @pl.when(core == 1)
    def _():
        waves(column_item, 5, 10)

    scale = HD ** (-0.5) * LOG2E
    row_at = lax.rem(lax.broadcasted_iota(jnp.int32, (2 * BLK, BLK), 0), BLK)
    col_at = lax.broadcasted_iota(jnp.int32, (2 * BLK, BLK), 1)
    ones = jnp.ones((8 * BLK, BLK), jnp.bfloat16)
    lane = lax.broadcasted_iota(jnp.int32, (BLK, BLK), 1)
    sub = lax.broadcasted_iota(jnp.int32, (BLK, BLK), 0)

    def scores(r, row, diagonal):
        keys = buf[r, pl.ds(row * 8, 8)].reshape(8 * BLK, BLK)
        raw = lax.dot_general(
            q_ref[r], keys, (((1,), (1,)), ((), ())), preferred_element_type=jnp.float32
        )
        parts = []
        for i in range(8):
            part = raw[:, i * BLK : (i + 1) * BLK] * scale + bias_ref[r, row * 8 + i]
            if diagonal:
                part = jnp.where((col_at <= row_at) | (y != i), part, NEG)
            parts.append(part)
        return jnp.concatenate(parts, axis=1), jnp.concatenate([keys, ones], axis=1)

    def one_rank(r, carry):
        s, wide = scores(r, z, True)
        best = jnp.max(s, axis=1, keepdims=True)
        p = jnp.exp2(s - best).astype(jnp.bfloat16)
        top[...] = best
        acc[...] = jnp.dot(p, wide, preferred_element_type=jnp.float32)

        def one_row(i, carry):
            s, wide = scores(r, z - 1 - i, False)
            old = top[...]
            best = jnp.maximum(old, jnp.max(s, axis=1, keepdims=True))
            p = jnp.exp2(s - best).astype(jnp.bfloat16)
            top[...] = best
            acc[...] = acc[...] * jnp.exp2(old - best) + jnp.dot(
                p, wide, preferred_element_type=jnp.float32
            )
            return carry

        lax.fori_loop(0, z, one_row, 0)
        full = acc[:, 0:128] / acc[:, 128:256]
        both = jnp.where(lane < HD, pltpu.roll(full[0:BLK], HD, 1), full[BLK:])
        both = jnp.where(sub + block * BLK < meta_ref[1, r], both, 0.0)
        att[r, :, pl.ds(pl.multiple_of(member * BLK, BLK), BLK)] = both.astype(jnp.bfloat16)
        return carry

    lax.fori_loop(0, mine, one_rank, 0)

    def share(chip, which, k, half, slot, target):
        lo, hi = {0: (0, k), 1: (0, k // 2), 2: (k // 2, k)}[half]
        t = lax.rem(chip + 4, 4) * 2 + which
        part = att.at[lo:hi, :, pl.ds(pl.multiple_of(t * BLK, BLK), BLK)]
        return pltpu.make_async_remote_copy(
            src_ref=part, dst_ref=part, send_sem=tp_send.at[slot], recv_sem=tp_recv.at[slot],
            device_id=target, device_id_type=MESH,
        )

    right, left, sibling = at_tp(x + 1, core), at_tp(x - 1, core), at_tp(x, 1 - core)

    def tp_steps(k):
        def go(chip, half, slot, target):
            if half == 1 and k < 2:
                return
            share(chip, core, k, half, slot, target).start()

        def got(chip, which, half, slot):
            if half == 1 and k < 2:
                return
            share(chip, which, k, half, slot, right).wait_recv()

        def done(half, slot):
            if half == 1 and k < 2:
                return
            share(x, core, k, half, slot, right).wait_send()

        go(x, 0, 0, right)
        go(x, 0, 1, left)
        go(x, 0, 2, sibling)
        got(x - 1, core, 0, 0)
        go(x - 1, 1, 3, right)
        go(x - 1, 0, 5, sibling)
        got(x + 1, core, 0, 1)
        go(x + 1, 2, 4, left)
        go(x + 1, 0, 6, sibling)
        got(x - 2, core, 1, 3)
        go(x - 2, 1, 7, sibling)
        got(x + 2, core, 2, 4)
        go(x + 2, 2, 8, sibling)
        got(x, 1 - core, 0, 2)
        got(x - 1, 1 - core, 0, 5)
        got(x + 1, 1 - core, 0, 6)
        got(x - 2, 1 - core, 1, 7)
        got(x + 2, 1 - core, 2, 8)
        for half, slot in ((0, 0), (0, 1), (0, 2), (1, 3), (2, 4), (0, 5), (0, 6), (1, 7), (2, 8)):
            done(half, slot)

    each_size(mine, tp_steps)

    @pl.when(core == 0)
    def _():
        drain(row_item, 8)

    @pl.when(core == 1)
    def _():
        drain(column_item, 5)

    result = pltpu.make_async_copy(att, out_ref, out_sem)
    result.start()
    result.wait()


def exchange(bias, meta, queries, keyvals):
    smem = pl.BlockSpec(memory_space=pltpu.SMEM)
    vmem = pl.BlockSpec(memory_space=pltpu.VMEM)
    return pl.pallas_call(
        functools.partial(exchange_kernel, RANKS),
        name="exchange",
        out_shape=jax.ShapeDtypeStruct((SEQS, BLK, 1024), jnp.bfloat16),
        in_specs=[smem, smem, vmem, vmem],
        out_specs=pl.BlockSpec(memory_space=pl.ANY),
        scratch_shapes=[
            pltpu.VMEM((SEQS, 64, BLK, BLK), jnp.bfloat16),
            pltpu.VMEM((SEQS, BLK, 1024), jnp.bfloat16),
            pltpu.VMEM((2 * BLK, 2 * BLK), jnp.float32),
            pltpu.VMEM((2 * BLK, 1), jnp.float32),
            pltpu.SemaphoreType.DMA,
            pltpu.SemaphoreType.DMA((64,)),
            pltpu.SemaphoreType.DMA((2, 64)),
            pltpu.SemaphoreType.DMA((2, 64)),
            pltpu.SemaphoreType.DMA((9,)),
            pltpu.SemaphoreType.DMA((9,)),
            pltpu.SemaphoreType.DMA,
        ],
        compiler_params=pltpu.CompilerParams(
            collective_id=0, has_side_effects=True, vmem_limit_bytes=48 * 1024 * 1024
        ),
    )(bias, meta, queries, keyvals)


def finish_kernel(meta_ref, att_ref, w_ref, out_ref, att_buf, sems):
    first = lax.axis_index("kv") * BLK

    def fetch(r):
        return pltpu.make_async_copy(att_ref.at[r], att_buf.at[r], sems.at[r])

    for r in range(SEQS):
        fetch(r).start()
    for r in range(SEQS):
        fetch(r).wait()
        s = meta_ref[0, r]
        live = meta_ref[1, r] > first

        @pl.when(live)
        def _():
            out_ref[s] = jnp.dot(
                att_buf[r], w_ref[...], preferred_element_type=jnp.float32
            ).astype(jnp.bfloat16)

        @pl.when(jnp.logical_not(live))
        def _():
            out_ref[s] = jnp.zeros((BLK, 256), jnp.bfloat16)


def finish(meta, attended, w_output):
    vmem = pl.BlockSpec(memory_space=pltpu.VMEM)
    return pl.pallas_call(
        finish_kernel,
        name="finish",
        out_shape=jax.ShapeDtypeStruct((SEQS, BLK, 256), jnp.bfloat16),
        in_specs=[pl.BlockSpec(memory_space=pltpu.SMEM), pl.BlockSpec(memory_space=pl.ANY), vmem],
        out_specs=vmem,
        scratch_shapes=[
            pltpu.VMEM((SEQS, BLK, 1024), jnp.bfloat16),
            pltpu.SemaphoreType.DMA((SEQS,)),
        ],
        compiler_params=pltpu.CompilerParams(vmem_limit_bytes=16 * 1024 * 1024),
    )(meta, attended, w_output)


def per_device(tokens, w_query, w_key, w_value, w_output, chosen, lengths):
    queries, keyvals, bias, meta = project(
        lengths, chosen[:, 0, :], tokens, w_query, w_key, w_value
    )
    attended = exchange(bias, meta, queries, keyvals)
    return finish(meta, attended, w_output)


def solution(mesh):
    return jax.shard_map(
        per_device,
        mesh=mesh,
        in_specs=(
            P(None, "kv", None),
            P(None, "tp"),
            P(None, "tp"),
            P(None, "tp"),
            P(None, "tp"),
            P(None, "kv", None),
            P(),
        ),
        out_specs=P(None, "kv", "tp"),
        check_vma=False,
    )
```

```python
import functools

import jax
import jax.numpy as jnp
from jax import lax
from jax.experimental import pallas as pl
from jax.experimental.pallas import tpu as pltpu
from jax.sharding import PartitionSpec as P

SEQS = 8
BLK = 128
SEL = 32
HD = 64
MESH = pl.DeviceIdType.MESH
LOG2E = 1.4426950408889634
NEG = -1e30
GROUPS = ((0, 2), (2, 2), (4, 1), (5, 3))
SKEW = (0, 0, 1, 1)
UPTO = (3, 4, 5, 7, 7, 7, 7, 7)
FULL = ((8, 8, 7, 5, 4, 3, 3, 2), (8, 7, 4, 3))
LIGHT = ((8, 8, 5, 4, 2, 2, 2, 1), (8, 4, 3, 2))


def project_kernel(
    len_ref, chosen_ref, tok_ref, wq_ref, wk_ref, wv_ref,
    q_ref, kv_ref, bias_ref, meta_ref, tok_buf, w_buf, wt_buf, row_buf, sems, w_sems,
):
    block = lax.axis_index("kv")
    first = block * BLK
    weights = (
        pltpu.make_async_copy(wk_ref, wt_buf.at[0:HD], w_sems.at[0]),
        pltpu.make_async_copy(wv_ref, wt_buf.at[HD : 2 * HD], w_sems.at[1]),
        pltpu.make_async_copy(wq_ref, w_buf.at[:, 0:128], w_sems.at[2]),
    )
    for copy in weights:
        copy.start()
    for s in range(SEQS):
        rank = jnp.int32(0)
        for t in range(SEQS):
            if t != s:
                ahead = len_ref[t] > len_ref[s] if t > s else len_ref[t] >= len_ref[s]
                rank = rank + ahead.astype(jnp.int32)
        meta_ref[0, rank] = jnp.int32(s)
        meta_ref[1, rank] = len_ref[s]
    light = jnp.int32(1)
    for row, most in enumerate(LIGHT[0]):
        if most < SEQS:
            light = jnp.where(meta_ref[1, most] > 8 * BLK * row, 0, light)
    for i in range(SEQS):
        meta_ref[2, i] = light

    def fetch(r):
        return pltpu.make_async_copy(tok_ref.at[meta_ref[0, r]], tok_buf.at[r], sems.at[r])

    for r in range(SEQS):
        fetch(r).start()
    for r in range(SEQS):
        row_buf[r : r + 1] = chosen_ref[pl.ds(meta_ref[0, r], 1)]
    picked = row_buf[...]
    for c in range(64):
        listed = jnp.max(jnp.where(picked == c, 0.0, NEG), axis=1, keepdims=True)
        bias_ref[:, c * BLK : (c + 1) * BLK] = jnp.broadcast_to(listed, (SEQS, BLK))
    weights[0].wait()
    weights[1].wait()
    w_buf[:, 128:256] = wt_buf[...].T
    weights[2].wait()
    lane = lax.broadcasted_iota(jnp.int32, (BLK, 128), 1)
    for g in range(SEQS // 2):
        for r in (2 * g, 2 * g + 1):
            fetch(r).wait()
        live = meta_ref[1, 2 * g] > first

        @pl.when(live)
        def _():
            rows = tok_buf[2 * g : 2 * g + 2].reshape(2 * BLK, -1)
            out = jnp.dot(rows, w_buf[...], preferred_element_type=jnp.float32)
            for i in range(2):
                part = out[i * BLK : (i + 1) * BLK]
                q = part[:, 0:128]
                q_ref[2 * g + i, 0:128] = jnp.where(lane < HD, q, 0.0).astype(jnp.bfloat16)
                q_ref[2 * g + i, 128:256] = jnp.where(
                    lane < HD, pltpu.roll(q, HD, 1), 0.0
                ).astype(jnp.bfloat16)
                kv_ref[2 * g + i] = part[:, 128:256].astype(jnp.bfloat16)

        @pl.when(jnp.logical_not(live))
        def _():
            q_ref[2 * g : 2 * g + 2] = jnp.zeros((2, 2 * BLK, 128), jnp.bfloat16)
            kv_ref[2 * g : 2 * g + 2] = jnp.zeros((2, BLK, 128), jnp.bfloat16)


def project(lengths, picked, tokens, w_query, w_key, w_value):
    smem = pl.BlockSpec(memory_space=pltpu.SMEM)
    vmem = pl.BlockSpec(memory_space=pltpu.VMEM)
    hbm = pl.BlockSpec(memory_space=pltpu.HBM)
    return pl.pallas_call(
        project_kernel,
        name="project",
        out_shape=(
            jax.ShapeDtypeStruct((SEQS, 2 * BLK, 128), jnp.bfloat16),
            jax.ShapeDtypeStruct((SEQS, BLK, 128), jnp.bfloat16),
            jax.ShapeDtypeStruct((SEQS, 64 * BLK), jnp.float32),
            jax.ShapeDtypeStruct((3, SEQS), jnp.int32),
        ),
        in_specs=[smem, vmem, hbm, hbm, hbm, hbm],
        out_specs=(vmem, vmem, vmem, smem),
        scratch_shapes=[
            pltpu.VMEM((SEQS, BLK, 2048), jnp.bfloat16),
            pltpu.VMEM((2048, 256), jnp.bfloat16),
            pltpu.VMEM((2 * HD, 2048), jnp.bfloat16),
            pltpu.VMEM((SEQS, SEL), jnp.int32),
            pltpu.SemaphoreType.DMA((SEQS,)),
            pltpu.SemaphoreType.DMA((3,)),
        ],
    )(lengths, picked, tokens, w_query, w_key.T, w_value.T)


def nibble(table):
    packed = sum(v << (4 * i) for i, v in enumerate(table))

    def look(index):
        return (jnp.int32(packed) >> (4 * index)) & 15

    return look


def hop_count(at, row):
    return at - row if at <= UPTO[row] else 8 - at


def exchange_kernel(
    plan, bias_ref, meta_ref, q_ref, kv_ref, att,
    buf, acc, top, own_sem, recv, send, tp_recv, tp_send,
):
    ranks, reach = plan
    ranks_at, upto_at = nibble(ranks), nibble(UPTO)
    hops_max_at = nibble([max(hop_count(at, row) for row in range(at + 1)) for at in range(8)])
    block = lax.axis_index("kv")
    member = lax.axis_index("tp")
    z, y = block >> 3, block & 7
    x, core = member >> 1, member & 1
    mine = ranks_at(z)
    first_core = core == 0

    def at_kv(row, col):
        return {"kv": (row & 7) * 8 + (col & 7)}

    def at_tp(chip, which):
        return {"tp": (chip & 3) * 2 + which}

    own = pltpu.make_async_copy(kv_ref, buf.at[:, block], own_sem)
    own.start()
    barrier = pltpu.get_barrier_semaphore()

    def greet(target):
        pl.semaphore_signal(barrier, inc=1, device_id=target, device_id_type=MESH)

    for target in (
        at_kv(z, y + 1), at_kv(z, y - 1),
        at_tp(x + 1, core), at_tp(x - 1, core), at_tp(x, 1 - core),
    ):
        greet(target)
    for step in (1, 2, 6, 7):
        greet(at_kv(z + step, y))

    @pl.when(z == 2)
    def _():
        greet(at_kv(jnp.int32(7), y))

    @pl.when(z == 7)
    def _():
        greet(at_kv(jnp.int32(2), y))

    pl.semaphore_wait(barrier, jnp.where((z == 2) | (z == 7), 10, 9))
    own.wait()

    def link(g, c, sem, target):
        lo, count = GROUPS[g]
        part = buf.at[lo : lo + count, c]
        return pltpu.make_async_remote_copy(
            src_ref=part, dst_ref=part, send_sem=sem, recv_sem=recv.at[g, c],
            device_id=target, device_id_type=MESH,
        )

    def to_right(g, c, row):
        link(g, c, send.at[0, g, row], at_kv(z, y + 1)).start()

    def to_left(g, c, row):
        link(g, c, send.at[1, g, row], at_kv(z, y - 1)).start()

    def arrived(g, c):
        link(g, c, send.at[0, 0, 0], at_kv(z, y + 1)).wait_recv()

    def route(row):
        upto = upto_at(row)
        rises = z <= upto
        hops = jnp.where(rises, z - row, 8 - z)
        return upto, rises, hops

    def needs(g, row, upto, rises):
        up = rises & (z < jnp.minimum(upto, reach[g] - 1))
        falls = upto + 1 < reach[g]
        wrap = (z == row) & falls
        down = jnp.logical_not(rises) & (z > upto + 1) & falls
        takes = (rises & (z < reach[g])) | (jnp.logical_not(rises) & falls)
        return takes, up, wrap, down

    def column(g, c, row, up, wrap, down):
        @pl.when(up)
        def _():
            link(g, c, send.at[2, g, row], at_kv(z + 1, y)).start()

        @pl.when(wrap)
        def _():
            link(g, c, send.at[3, g, row], at_kv(jnp.int32(7), y)).start()

        @pl.when(down)
        def _():
            link(g, c, send.at[3, g, row], at_kv(z - 1, y)).start()

    def row_items(u, row, upto, rises):
        for g in range(len(GROUPS)):
            step = u - SKEW[g]
            takes, up, wrap, down = needs(g, row, upto, rises)
            in_row = row == z

            @pl.when((step >= 0) & (step < 5) & takes)
            def _(g=g, step=step, up=up, wrap=wrap, down=down, in_row=in_row):
                c = row * 8 + ((y - step) & 7)

                @pl.when(jnp.logical_not(in_row & (step == 0)))
                def _():
                    arrived(g, c)

                @pl.when(in_row & (step < 4))
                def _():
                    to_right(g, c, row)

                @pl.when(in_row & (step == 0))
                def _():
                    to_left(g, c, row)

                column(g, c, row, up, wrap, down)

                @pl.when((step > 0) & (step < 4))
                def _():
                    c = row * 8 + ((y + step) & 7)
                    arrived(g, c)

                    @pl.when(in_row & (step < 3))
                    def _():
                        to_left(g, c, row)

                    column(g, c, row, up, wrap, down)

    def column_items(t, row):
        away = z - row
        far = (away + 1) >> 1
        for g in range(len(GROUPS)):
            step = t - far - SKEW[g]
            used = z < reach[g]

            @pl.when((step == 0) & used)
            def _(g=g):
                c = row * 8 + y

                @pl.when(row != z)
                def _():
                    arrived(g, c)

                to_right(g, c, row)
                to_left(g, c, row)

                for ahead in (1, 2):
                    @pl.when(((away & 1) == 0) & (z + ahead < reach[g]))
                    def _(ahead=ahead):
                        link(g, c, send.at[1 + ahead, g, row], at_kv(z + ahead, y)).start()

            @pl.when((step > 0) & (step < 5) & used)
            def _(g=g, step=step):
                c = row * 8 + ((y - step) & 7)
                arrived(g, c)

                @pl.when(step < 4)
                def _():
                    to_right(g, c, row)
                    c2 = row * 8 + ((y + step) & 7)
                    arrived(g, c2)

                    @pl.when(step < 3)
                    def _():
                        to_left(g, c2, row)

    scale = HD ** (-0.5) * LOG2E
    row_at = lax.broadcasted_iota(jnp.int32, (2 * BLK, BLK), 0) & (BLK - 1)
    col_at = lax.broadcasted_iota(jnp.int32, (2 * BLK, BLK), 1)
    ones = jnp.ones((8 * BLK, BLK), jnp.bfloat16)
    lane = lax.broadcasted_iota(jnp.int32, (BLK, BLK), 1)
    sub = lax.broadcasted_iota(jnp.int32, (BLK, BLK), 0)

    def scores(r, row):
        keys = buf[r, pl.ds(row * 8, 8)].reshape(8 * BLK, BLK)
        raw = lax.dot_general(
            q_ref[r], keys, (((1,), (1,)), ((), ())), preferred_element_type=jnp.float32
        )
        bias = bias_ref[pl.ds(r, 1), pl.ds(pl.multiple_of(row * 8 * BLK, 8 * BLK), 8 * BLK)]
        return raw * scale + bias, jnp.concatenate([keys, ones], axis=1)

    def attend(r, row):
        @pl.when(row == z)
        def _():
            s, wide = scores(r, row)
            parts = []
            for i in range(8):
                part = s[:, i * BLK : (i + 1) * BLK]
                parts.append(jnp.where((col_at <= row_at) | (y != i), part, NEG))
            s = jnp.concatenate(parts, axis=1)
            best = jnp.max(s, axis=1, keepdims=True)
            p = jnp.exp2(s - best).astype(jnp.bfloat16)
            top[r] = best
            acc[r] = jnp.dot(p, wide, preferred_element_type=jnp.float32)

        @pl.when(row != z)
        def _():
            s, wide = scores(r, row)
            old = top[r]
            best = jnp.maximum(old, jnp.max(s, axis=1, keepdims=True))
            p = jnp.exp2(s - best).astype(jnp.bfloat16)
            top[r] = best
            acc[r] = acc[r] * jnp.exp2(old - best) + jnp.dot(
                p, wide, preferred_element_type=jnp.float32
            )

    def settle(r):
        total = acc[r]
        full = total[:, 0:128] / total[:, 128:256]
        both = jnp.where(lane < HD, pltpu.roll(full[0:BLK], HD, 1), full[BLK:])
        both = jnp.where(sub + block * BLK < meta_ref[1, r], both, 0.0)
        att[member, r] = both.astype(jnp.bfloat16)

    def share(g, chip, which, slot, target):
        t = (chip & 3) * 2 + which
        lo, count = GROUPS[g]
        part = att.at[t, lo : lo + count]
        return pltpu.make_async_remote_copy(
            src_ref=part, dst_ref=part, send_sem=tp_send.at[g, slot], recv_sem=tp_recv.at[g, slot],
            device_id=target, device_id_type=MESH,
        )

    right, left, sibling = at_tp(x + 1, core), at_tp(x - 1, core), at_tp(x, 1 - core)

    def share_own(g):
        share(g, x, core, 0, right).start()
        share(g, x, core, 1, left).start()
        share(g, x, core, 2, sibling).start()

    def share_next(g):
        share(g, x - 1, core, 0, right).wait_recv()
        if g % 2 == 0:
            share(g, x - 1, core, 3, right).start()
        share(g, x - 1, core, 4, sibling).start()
        share(g, x + 1, core, 1, right).wait_recv()
        if g % 2 == 1:
            share(g, x + 1, core, 3, left).start()
        share(g, x + 1, core, 5, sibling).start()

    def share_far(g):
        share(g, x + 2, core, 3, right).wait_recv()
        share(g, x + 2, core, 6, sibling).start()

    last = len(GROUPS) - 1
    farthest = jnp.where(first_core, hops_max_at(z), (z + 1) >> 1)

    def delay_of(row):
        return jnp.where(first_core, route(row)[2], (z - row + 1) >> 1)


    def wave(t, carry):
        def comm(i, carry):
            row = z - i
            upto, rises, hops = route(row)
            u = t - hops

            @pl.when(first_core)
            def _():
                row_items(u, row, upto, rises)

            @pl.when(jnp.logical_not(first_core))
            def _():
                column_items(t, row)

            return carry

        lax.fori_loop(0, z + 1, comm, 0)

        def matching(at):
            lo, hi = jnp.int32(8), jnp.int32(0)
            for g, (first, count) in enumerate(GROUPS):
                hit = at == SKEW[g] + 4
                lo = jnp.where(hit, jnp.minimum(lo, first), lo)
                hi = jnp.where(hit, jnp.maximum(hi, first + count), hi)
            return lo, jnp.minimum(hi, mine)

        def compute(i, carry):
            row = z - i
            lo, hi = matching(t - delay_of(row))

            def one(r, carry):
                attend(r, row)
                return carry

            @pl.when(delay_of(row) < farthest)
            def _():
                lax.fori_loop(lo, hi, one, 0)

            return carry

        lax.fori_loop(0, z + 1, compute, 0)
        lo, hi = matching(t - farthest)

        def close(r, carry):
            def one(i, carry):
                row = z - i

                @pl.when(delay_of(row) == farthest)
                def _():
                    attend(r, row)

                return carry

            lax.fori_loop(0, z + 1, one, 0)
            settle(r)
            for g, (first, count) in enumerate(GROUPS):
                @pl.when((r >= first) & (r == jnp.minimum(first + count, mine) - 1))
                def _(g=g):
                    share_own(g)
                    if g > 0:
                        share_next(g - 1)
                    if g > 1:
                        share_far(g - 2)

            return carry

        lax.fori_loop(lo, hi, close, 0)
        return carry

    lax.fori_loop(0, farthest + 5 + SKEW[last], wave, 0)
    for g, (first, count) in enumerate(GROUPS):
        @pl.when((mine > first) & (mine <= first + count))
        def _(g=g):
            share_next(g)
            if g > 0:
                share_far(g - 1)
            share_far(g)

    def sent(direction, g, row, columns):
        lo, count = GROUPS[g]
        part = buf.at[lo : lo + count, 0:columns]
        pltpu.make_async_remote_copy(
            src_ref=part, dst_ref=part, send_sem=send.at[direction, g, row],
            recv_sem=recv.at[0, 0], device_id=right, device_id_type=MESH,
        ).wait_send()

    def drain(row, carry):
        upto, rises, _ = route(row)
        for g in range(len(GROUPS)):
            _, up, wrap, down = needs(g, row, upto, rises)
            ring = (z < reach[g]) & (jnp.logical_not(first_core) | (row == z))

            @pl.when(ring)
            def _(g=g):
                sent(0, g, row, 4)
                sent(1, g, row, 3)

            for direction, used in ((2, up), (3, wrap | down)):
                @pl.when(used & first_core)
                def _(g=g, direction=direction):
                    sent(direction, g, row, 8)

            for ahead in (1, 2):
                straight = jnp.logical_not(first_core) & (((z - row) & 1) == 0)

                @pl.when(straight & (z < reach[g]) & (z + ahead < reach[g]))
                def _(g=g, ahead=ahead):
                    sent(1 + ahead, g, row, 1)

        return carry

    lax.fori_loop(0, z + 1, drain, 0)

    for g in range(len(GROUPS)):
        @pl.when(mine > GROUPS[g][0])
        def _(g=g):
            for chip, slot in ((x, 2), (x - 1, 4), (x + 1, 5), (x + 2, 6)):
                share(g, chip, 1 - core, slot, right).wait_recv()
            for slot in range(7):
                share(g, x, core, slot, right).wait_send()


def exchange(plan, collective, bias, meta, queries, keyvals):
    smem = pl.BlockSpec(memory_space=pltpu.SMEM)
    vmem = pl.BlockSpec(memory_space=pltpu.VMEM)
    return pl.pallas_call(
        functools.partial(exchange_kernel, plan),
        name="exchange",
        out_shape=jax.ShapeDtypeStruct((8, SEQS, BLK, BLK), jnp.bfloat16),
        in_specs=[vmem, smem, vmem, vmem],
        out_specs=vmem,
        scratch_shapes=[
            pltpu.VMEM((SEQS, 64, BLK, BLK), jnp.bfloat16),
            pltpu.VMEM((SEQS, 2 * BLK, 2 * BLK), jnp.float32),
            pltpu.VMEM((SEQS, 2 * BLK, 1), jnp.float32),
            pltpu.SemaphoreType.DMA,
            pltpu.SemaphoreType.DMA((len(GROUPS), 64)),
            pltpu.SemaphoreType.DMA((4, len(GROUPS), 8)),
            pltpu.SemaphoreType.DMA((len(GROUPS), 7)),
            pltpu.SemaphoreType.DMA((len(GROUPS), 7)),
        ],
        compiler_params=pltpu.CompilerParams(
            collective_id=collective, has_side_effects=True, vmem_limit_bytes=48 * 1024 * 1024
        ),
    )(bias, meta, queries, keyvals)


def finish_kernel(meta_ref, att_ref, w_ref, out_ref, att_buf, sems):
    first = lax.axis_index("kv") * BLK

    def fetch(r):
        return pltpu.make_async_copy(att_ref.at[:, r], att_buf.at[r], sems.at[r])

    for r in range(SEQS):
        fetch(r).start()
    for r in range(SEQS):
        fetch(r).wait()
        s = meta_ref[0, r]
        live = meta_ref[1, r] > first

        @pl.when(live)
        def _():
            rows = jnp.concatenate([att_buf[r, t] for t in range(8)], axis=1)
            out_ref[s] = jnp.dot(
                rows, w_ref[...], preferred_element_type=jnp.float32
            ).astype(jnp.bfloat16)

        @pl.when(jnp.logical_not(live))
        def _():
            out_ref[s] = jnp.zeros((BLK, 256), jnp.bfloat16)


def finish(meta, attended, w_output):
    vmem = pl.BlockSpec(memory_space=pltpu.VMEM)
    return pl.pallas_call(
        finish_kernel,
        name="finish",
        out_shape=jax.ShapeDtypeStruct((SEQS, BLK, 256), jnp.bfloat16),
        in_specs=[pl.BlockSpec(memory_space=pltpu.SMEM), pl.BlockSpec(memory_space=pl.ANY), vmem],
        out_specs=vmem,
        scratch_shapes=[
            pltpu.VMEM((SEQS, 8, BLK, BLK), jnp.bfloat16),
            pltpu.SemaphoreType.DMA((SEQS,)),
        ],
        compiler_params=pltpu.CompilerParams(vmem_limit_bytes=16 * 1024 * 1024),
    )(meta, attended, w_output)


def per_device(tokens, w_query, w_key, w_value, w_output, chosen, lengths):
    queries, keyvals, bias, meta = project(
        lengths, chosen[:, 0, :], tokens, w_query, w_key, w_value
    )
    attended = lax.cond(
        meta[2, 0] > 0,
        functools.partial(exchange, LIGHT, 0),
        functools.partial(exchange, FULL, 1),
        bias, meta, queries, keyvals,
    )
    return finish(meta, attended, w_output)


def solution(mesh):
    return jax.shard_map(
        per_device,
        mesh=mesh,
        in_specs=(
            P(None, "kv", None),
            P(None, "tp"),
            P(None, "tp"),
            P(None, "tp"),
            P(None, "tp"),
            P(None, "kv", None),
            P(),
        ),
        out_specs=P(None, "kv", "tp"),
        check_vma=False,
    )
```

```python
import functools

import jax
import jax.numpy as jnp
from jax import lax
from jax.experimental import pallas as pl
from jax.experimental.pallas import tpu as pltpu
from jax.sharding import PartitionSpec as P

SEQS = 8
BLK = 128
SEL = 32
HD = 64
MESH = pl.DeviceIdType.MESH
LOG2E = 1.4426950408889634
NEG = -1e30
GROUPS = ((0, 2), (2, 2), (4, 1), (5, 3))
SKEW = (0, 0, 1, 2)
SIDE = (1, -1, -1, 1)
STRAIGHT = (True, True, True, True)
UPTO = (3, 4, 5, 7, 7, 7, 7, 7)
FULL = ((8, 8, 7, 5, 4, 3, 3, 2), (8, 7, 4, 3))
LIGHT = ((8, 8, 5, 4, 2, 2, 2, 1), (8, 4, 3, 2))


def project_kernel(
    len_ref, chosen_ref, tok_ref, wq_ref, wk_ref, wv_ref,
    q_ref, kv_ref, bias_ref, meta_ref, tok_buf, w_buf, wt_buf, row_buf, sems, w_sems,
):
    block = lax.axis_index("kv")
    first = block * BLK
    weights = (
        pltpu.make_async_copy(wk_ref, wt_buf.at[0:HD], w_sems.at[0]),
        pltpu.make_async_copy(wv_ref, wt_buf.at[HD : 2 * HD], w_sems.at[1]),
        pltpu.make_async_copy(wq_ref, w_buf.at[:, 0:128], w_sems.at[2]),
    )
    for copy in weights:
        copy.start()
    for s in range(SEQS):
        rank = jnp.int32(0)
        for t in range(SEQS):
            if t != s:
                ahead = len_ref[t] > len_ref[s] if t > s else len_ref[t] >= len_ref[s]
                rank = rank + ahead.astype(jnp.int32)
        meta_ref[0, rank] = jnp.int32(s)
        meta_ref[1, rank] = len_ref[s]
    light = jnp.int32(1)
    for row, most in enumerate(LIGHT[0]):
        if most < SEQS:
            light = jnp.where(meta_ref[1, most] > 8 * BLK * row, 0, light)
    for i in range(SEQS):
        meta_ref[2, i] = light

    def fetch(r):
        return pltpu.make_async_copy(tok_ref.at[meta_ref[0, r]], tok_buf.at[r], sems.at[r])

    for r in range(SEQS):
        fetch(r).start()
    for r in range(SEQS):
        row_buf[r : r + 1] = chosen_ref[pl.ds(meta_ref[0, r], 1)]
    picked = row_buf[...]
    for c in range(64):
        listed = jnp.max(jnp.where(picked == c, 0.0, NEG), axis=1, keepdims=True)
        bias_ref[:, c * BLK : (c + 1) * BLK] = jnp.broadcast_to(listed, (SEQS, BLK))
    weights[0].wait()
    weights[1].wait()
    w_buf[:, 128:256] = wt_buf[...].T
    weights[2].wait()
    lane = lax.broadcasted_iota(jnp.int32, (BLK, 128), 1)
    for g in range(SEQS // 2):
        for r in (2 * g, 2 * g + 1):
            fetch(r).wait()
        live = meta_ref[1, 2 * g] > first

        @pl.when(live)
        def _():
            rows = tok_buf[2 * g : 2 * g + 2].reshape(2 * BLK, -1)
            out = jnp.dot(rows, w_buf[...], preferred_element_type=jnp.float32)
            for i in range(2):
                part = out[i * BLK : (i + 1) * BLK]
                q = part[:, 0:128]
                q_ref[2 * g + i, 0:128] = jnp.where(lane < HD, q, 0.0).astype(jnp.bfloat16)
                q_ref[2 * g + i, 128:256] = jnp.where(
                    lane < HD, pltpu.roll(q, HD, 1), 0.0
                ).astype(jnp.bfloat16)
                kv_ref[2 * g + i] = part[:, 128:256].astype(jnp.bfloat16)

        @pl.when(jnp.logical_not(live))
        def _():
            q_ref[2 * g : 2 * g + 2] = jnp.zeros((2, 2 * BLK, 128), jnp.bfloat16)
            kv_ref[2 * g : 2 * g + 2] = jnp.zeros((2, BLK, 128), jnp.bfloat16)


def project(lengths, picked, tokens, w_query, w_key, w_value):
    smem = pl.BlockSpec(memory_space=pltpu.SMEM)
    vmem = pl.BlockSpec(memory_space=pltpu.VMEM)
    hbm = pl.BlockSpec(memory_space=pltpu.HBM)
    return pl.pallas_call(
        project_kernel,
        name="project",
        out_shape=(
            jax.ShapeDtypeStruct((SEQS, 2 * BLK, 128), jnp.bfloat16),
            jax.ShapeDtypeStruct((SEQS, BLK, 128), jnp.bfloat16),
            jax.ShapeDtypeStruct((SEQS, 64 * BLK), jnp.float32),
            jax.ShapeDtypeStruct((3, SEQS), jnp.int32),
        ),
        in_specs=[smem, vmem, hbm, hbm, hbm, hbm],
        out_specs=(vmem, vmem, vmem, smem),
        scratch_shapes=[
            pltpu.VMEM((SEQS, BLK, 2048), jnp.bfloat16),
            pltpu.VMEM((2048, 256), jnp.bfloat16),
            pltpu.VMEM((2 * HD, 2048), jnp.bfloat16),
            pltpu.VMEM((SEQS, SEL), jnp.int32),
            pltpu.SemaphoreType.DMA((SEQS,)),
            pltpu.SemaphoreType.DMA((3,)),
        ],
    )(lengths, picked, tokens, w_query, w_key.T, w_value.T)


def nibble(table):
    packed = sum(v << (4 * i) for i, v in enumerate(table))

    def look(index):
        return (jnp.int32(packed) >> (4 * index)) & 15

    return look


def hop_count(at, row):
    return at - row if at <= UPTO[row] else 8 - at


def exchange_kernel(
    plan, bias_ref, meta_ref, q_ref, kv_ref, att,
    buf, acc, top, own_sem, recv, send, tp_recv, tp_send,
):
    ranks, reach = plan
    ranks_at, upto_at = nibble(ranks), nibble(UPTO)
    hops_max_at = nibble([max(hop_count(at, row) for row in range(at + 1)) for at in range(8)])
    block = lax.axis_index("kv")
    member = lax.axis_index("tp")
    z, y = block >> 3, block & 7
    x, core = member >> 1, member & 1
    mine = ranks_at(z)
    first_core = core == 0

    def at_kv(row, col):
        return {"kv": (row & 7) * 8 + (col & 7)}

    def at_tp(chip, which):
        return {"tp": (chip & 3) * 2 + which}

    own = pltpu.make_async_copy(kv_ref, buf.at[:, block], own_sem)
    own.start()
    barrier = pltpu.get_barrier_semaphore()

    def greet(target):
        pl.semaphore_signal(barrier, inc=1, device_id=target, device_id_type=MESH)

    for target in (
        at_kv(z, y + 1), at_kv(z, y - 1),
        at_tp(x + 1, core), at_tp(x - 1, core), at_tp(x + 2, core), at_tp(x, 1 - core),
    ):
        greet(target)
    for step in (1, 2, 6, 7):
        greet(at_kv(z + step, y))

    @pl.when(z == 2)
    def _():
        greet(at_kv(jnp.int32(7), y))

    @pl.when(z == 7)
    def _():
        greet(at_kv(jnp.int32(2), y))

    pl.semaphore_wait(barrier, jnp.where((z == 2) | (z == 7), 11, 10))
    own.wait()

    def link(g, c, sem, target):
        lo, count = GROUPS[g]
        part = buf.at[lo : lo + count, c]
        return pltpu.make_async_remote_copy(
            src_ref=part, dst_ref=part, send_sem=sem, recv_sem=recv.at[g, c],
            device_id=target, device_id_type=MESH,
        )

    def to_long(g, c, row, side):
        link(g, c, send.at[0, g, row], at_kv(z, y + side)).start()

    def to_short(g, c, row, side):
        link(g, c, send.at[1, g, row], at_kv(z, y - side)).start()

    def arrived(g, c):
        link(g, c, send.at[0, 0, 0], at_kv(z, y + 1)).wait_recv()

    def route(row):
        upto = upto_at(row)
        rises = z <= upto
        hops = jnp.where(rises, z - row, 8 - z)
        return upto, rises, hops

    def needs(g, row, upto, rises):
        up = rises & (z < jnp.minimum(upto, reach[g] - 1))
        falls = upto + 1 < reach[g]
        wrap = (z == row) & falls
        down = jnp.logical_not(rises) & (z > upto + 1) & falls
        takes = (rises & (z < reach[g])) | (jnp.logical_not(rises) & falls)
        return takes, up, wrap, down

    def column(g, c, row, up, wrap, down):
        @pl.when(up)
        def _():
            link(g, c, send.at[2, g, row], at_kv(z + 1, y)).start()

        @pl.when(wrap)
        def _():
            link(g, c, send.at[3, g, row], at_kv(jnp.int32(7), y)).start()

        @pl.when(down)
        def _():
            link(g, c, send.at[3, g, row], at_kv(z - 1, y)).start()

    def row_items(u, row, upto, rises):
        for g in range(len(GROUPS)):
            step = u - SKEW[g]
            side = SIDE[g]
            takes, up, wrap, down = needs(g, row, upto, rises)
            in_row = row == z

            @pl.when((step >= 0) & (step < 5) & takes)
            def _(g=g, step=step, side=side, up=up, wrap=wrap, down=down, in_row=in_row):
                c = row * 8 + ((y - side * step) & 7)

                @pl.when(jnp.logical_not(in_row & (step == 0)))
                def _():
                    arrived(g, c)

                @pl.when(in_row & (step < 4))
                def _():
                    to_long(g, c, row, side)

                @pl.when(in_row & (step == 0))
                def _():
                    to_short(g, c, row, side)

                column(g, c, row, up, wrap, down)

                @pl.when((step > 0) & (step < 4))
                def _():
                    c = row * 8 + ((y + side * step) & 7)
                    arrived(g, c)

                    @pl.when(in_row & (step < 3))
                    def _():
                        to_short(g, c, row, side)

                    column(g, c, row, up, wrap, down)

    def column_items(t, row):
        away = z - row
        far = (away + 1) >> 1
        for g in range(len(GROUPS)):
            step = t - far - SKEW[g]
            used = z < reach[g]
            side = SIDE[g] * (1 - 2 * (row & 1))

            @pl.when((step == 0) & used)
            def _(g=g, side=side):
                c = row * 8 + y

                @pl.when(row != z)
                def _():
                    arrived(g, c)

                to_long(g, c, row, side)
                to_short(g, c, row, side)

                for ahead in (1, 2):
                    @pl.when(((away & 1) == 0) & (z + ahead < reach[g]))
                    def _(ahead=ahead):
                        link(g, c, send.at[1 + ahead, g, row], at_kv(z + ahead, y)).start()

            @pl.when((step > 0) & (step < 5) & used)
            def _(g=g, step=step, side=side):
                c = row * 8 + ((y - side * step) & 7)
                arrived(g, c)

                @pl.when(step < 4)
                def _():
                    to_long(g, c, row, side)
                    c2 = row * 8 + ((y + side * step) & 7)
                    arrived(g, c2)

                    @pl.when(step < 3)
                    def _():
                        to_short(g, c2, row, side)

    scale = HD ** (-0.5) * LOG2E
    ones = jnp.ones((8 * BLK, BLK), jnp.bfloat16)
    lane = lax.broadcasted_iota(jnp.int32, (BLK, BLK), 1)
    sub = lax.broadcasted_iota(jnp.int32, (BLK, BLK), 0)

    def scores(r, row, rows, keys):
        raw = lax.dot_general(
            q_ref[r, rows], keys, (((1,), (1,)), ((), ())), preferred_element_type=jnp.float32
        )
        bias = bias_ref[pl.ds(r, 1), pl.ds(pl.multiple_of(row * 8 * BLK, 8 * BLK), 8 * BLK)]
        return raw * scale + bias

    def attend(r, row):
        @pl.when(row == z)
        def _():
            keys = buf[r, pl.ds(row * 8, 8)].reshape(8 * BLK, BLK)
            wide = jnp.concatenate([keys, ones], axis=1)
            for rows in (slice(0, BLK), slice(BLK, 2 * BLK)):
                s = scores(r, row, rows, keys)
                parts = []
                for i in range(8):
                    part = s[:, i * BLK : (i + 1) * BLK]
                    parts.append(jnp.where((lane <= sub) | (y != i), part, NEG))
                s = jnp.concatenate(parts, axis=1)
                best = jnp.max(s, axis=1, keepdims=True)
                p = jnp.exp2(s - best).astype(jnp.bfloat16)
                top[r, rows] = best
                acc[r, rows] = jnp.dot(p, wide, preferred_element_type=jnp.float32)

        @pl.when(row != z)
        def _():
            keys = buf[r, pl.ds(row * 8, 8)].reshape(8 * BLK, BLK)
            wide = jnp.concatenate([keys, ones], axis=1)
            for rows in (slice(0, BLK), slice(BLK, 2 * BLK)):
                s = scores(r, row, rows, keys)
                old = top[r, rows]
                best = jnp.maximum(old, jnp.max(s, axis=1, keepdims=True))
                p = jnp.exp2(s - best).astype(jnp.bfloat16)
                top[r, rows] = best
                acc[r, rows] = acc[r, rows] * jnp.exp2(old - best) + jnp.dot(
                    p, wide, preferred_element_type=jnp.float32
                )

    def settle(r):
        total = acc[r]
        full = total[:, 0:128] / total[:, 128:256]
        both = jnp.where(lane < HD, pltpu.roll(full[0:BLK], HD, 1), full[BLK:])
        both = jnp.where(sub + block * BLK < meta_ref[1, r], both, 0.0)
        att[member, r] = both.astype(jnp.bfloat16)

    def share(g, chip, which, slot, target):
        t = (chip & 3) * 2 + which
        lo, count = GROUPS[g]
        part = att.at[t, lo : lo + count]
        return pltpu.make_async_remote_copy(
            src_ref=part, dst_ref=part, send_sem=tp_send.at[g, slot], recv_sem=tp_recv.at[g, slot],
            device_id=target, device_id_type=MESH,
        )

    right, left, sibling = at_tp(x + 1, core), at_tp(x - 1, core), at_tp(x, 1 - core)

    def share_own(g):
        share(g, x, core, 0, right).start()
        share(g, x, core, 1, left).start()
        share(g, x, core, 2, sibling).start()
        if STRAIGHT[g]:
            share(g, x, core, 3, at_tp(x + 2, core)).start()

    def share_next(g):
        share(g, x - 1, core, 0, right).wait_recv()
        if g % 2 == 0 and not STRAIGHT[g]:
            share(g, x - 1, core, 3, right).start()
        share(g, x - 1, core, 4, sibling).start()
        share(g, x + 1, core, 1, right).wait_recv()
        if g % 2 == 1 and not STRAIGHT[g]:
            share(g, x + 1, core, 3, left).start()
        share(g, x + 1, core, 5, sibling).start()

    def share_far(g):
        share(g, x + 2, core, 3, right).wait_recv()
        share(g, x + 2, core, 6, sibling).start()

    last = len(GROUPS) - 1
    farthest = jnp.where(first_core, hops_max_at(z), (z + 1) >> 1)

    def delay_of(row):
        return jnp.where(first_core, route(row)[2], (z - row + 1) >> 1)


    def wave(t, carry):
        def comm(i, carry):
            row = z - i
            upto, rises, hops = route(row)
            u = t - hops

            @pl.when(first_core)
            def _():
                row_items(u, row, upto, rises)

            @pl.when(jnp.logical_not(first_core))
            def _():
                column_items(t, row)

            return carry

        lax.fori_loop(0, z + 1, comm, 0)

        def matching(at):
            lo, hi = jnp.int32(8), jnp.int32(0)
            for g, (first, count) in enumerate(GROUPS):
                hit = at == SKEW[g] + 4
                lo = jnp.where(hit, jnp.minimum(lo, first), lo)
                hi = jnp.where(hit, jnp.maximum(hi, first + count), hi)
            return lo, jnp.minimum(hi, mine)

        def compute(i, carry):
            row = z - i
            lo, hi = matching(t - delay_of(row))

            def one(r, carry):
                attend(r, row)
                return carry

            @pl.when(delay_of(row) < farthest)
            def _():
                lax.fori_loop(lo, hi, one, 0)

            return carry

        lax.fori_loop(0, z + 1, compute, 0)
        lo, hi = matching(t - farthest)

        def close(r, carry):
            def one(i, carry):
                row = z - i

                @pl.when(delay_of(row) == farthest)
                def _():
                    attend(r, row)

                return carry

            lax.fori_loop(0, z + 1, one, 0)
            settle(r)
            for g, (first, count) in enumerate(GROUPS):
                @pl.when((r >= first) & (r == jnp.minimum(first + count, mine) - 1))
                def _(g=g):
                    share_own(g)
                    if g > 0:
                        share_next(g - 1)
                    if g > 1:
                        share_far(g - 2)

            return carry

        lax.fori_loop(lo, hi, close, 0)
        return carry

    lax.fori_loop(0, farthest + 5 + SKEW[last], wave, 0)
    for g, (first, count) in enumerate(GROUPS):
        @pl.when((mine > first) & (mine <= first + count))
        def _(g=g):
            share_next(g)
            if g > 0:
                share_far(g - 1)
            share_far(g)

    def sent(direction, g, row, columns):
        lo, count = GROUPS[g]
        part = buf.at[lo : lo + count, 0:columns]
        pltpu.make_async_remote_copy(
            src_ref=part, dst_ref=part, send_sem=send.at[direction, g, row],
            recv_sem=recv.at[0, 0], device_id=right, device_id_type=MESH,
        ).wait_send()

    def drain(row, carry):
        upto, rises, _ = route(row)
        for g in range(len(GROUPS)):
            _, up, wrap, down = needs(g, row, upto, rises)
            ring = (z < reach[g]) & (jnp.logical_not(first_core) | (row == z))

            @pl.when(ring)
            def _(g=g):
                sent(0, g, row, 4)
                sent(1, g, row, 3)

            for direction, used in ((2, up), (3, wrap | down)):
                @pl.when(used & first_core)
                def _(g=g, direction=direction):
                    sent(direction, g, row, 8)

            for ahead in (1, 2):
                straight = jnp.logical_not(first_core) & (((z - row) & 1) == 0)

                @pl.when(straight & (z < reach[g]) & (z + ahead < reach[g]))
                def _(g=g, ahead=ahead):
                    sent(1 + ahead, g, row, 1)

        return carry

    lax.fori_loop(0, z + 1, drain, 0)

    for g in range(len(GROUPS)):
        @pl.when(mine > GROUPS[g][0])
        def _(g=g):
            for chip, slot in ((x, 2), (x - 1, 4), (x + 1, 5), (x + 2, 6)):
                share(g, chip, 1 - core, slot, right).wait_recv()
            for slot in range(7):
                share(g, x, core, slot, right).wait_send()


def exchange(plan, collective, bias, meta, queries, keyvals):
    smem = pl.BlockSpec(memory_space=pltpu.SMEM)
    vmem = pl.BlockSpec(memory_space=pltpu.VMEM)
    return pl.pallas_call(
        functools.partial(exchange_kernel, plan),
        name="exchange",
        out_shape=jax.ShapeDtypeStruct((8, SEQS, BLK, BLK), jnp.bfloat16),
        in_specs=[vmem, smem, vmem, vmem],
        out_specs=vmem,
        scratch_shapes=[
            pltpu.VMEM((SEQS, 64, BLK, BLK), jnp.bfloat16),
            pltpu.VMEM((SEQS, 2 * BLK, 2 * BLK), jnp.float32),
            pltpu.VMEM((SEQS, 2 * BLK, 1), jnp.float32),
            pltpu.SemaphoreType.DMA,
            pltpu.SemaphoreType.DMA((len(GROUPS), 64)),
            pltpu.SemaphoreType.DMA((4, len(GROUPS), 8)),
            pltpu.SemaphoreType.DMA((len(GROUPS), 7)),
            pltpu.SemaphoreType.DMA((len(GROUPS), 7)),
        ],
        compiler_params=pltpu.CompilerParams(
            collective_id=collective, has_side_effects=True, vmem_limit_bytes=48 * 1024 * 1024
        ),
    )(bias, meta, queries, keyvals)


def finish_kernel(meta_ref, att_ref, w_ref, out_ref):
    first = lax.axis_index("kv") * BLK
    for r in range(0, SEQS, 2):
        @pl.when(meta_ref[1, r] > first)
        def _(r=r):
            rows = jnp.concatenate(
                [att_ref[t, r : r + 2].reshape(2 * BLK, BLK) for t in range(8)], axis=1
            )
            mixed = jnp.dot(rows, w_ref[...], preferred_element_type=jnp.float32)
            out_ref[meta_ref[0, r]] = mixed[:BLK].astype(jnp.bfloat16)
            kept = jnp.where(meta_ref[1, r + 1] > first, mixed[BLK:], 0.0)
            out_ref[meta_ref[0, r + 1]] = kept.astype(jnp.bfloat16)

        @pl.when(meta_ref[1, r] <= first)
        def _(r=r):
            for i in (r, r + 1):
                out_ref[meta_ref[0, i]] = jnp.zeros((BLK, 256), jnp.bfloat16)


def finish(meta, attended, w_output):
    vmem = pl.BlockSpec(memory_space=pltpu.VMEM)
    return pl.pallas_call(
        finish_kernel,
        name="finish",
        out_shape=jax.ShapeDtypeStruct((SEQS, BLK, 256), jnp.bfloat16),
        in_specs=[pl.BlockSpec(memory_space=pltpu.SMEM), vmem, vmem],
        out_specs=vmem,
        compiler_params=pltpu.CompilerParams(vmem_limit_bytes=16 * 1024 * 1024),
    )(meta, attended, w_output)


def per_device(tokens, w_query, w_key, w_value, w_output, chosen, lengths):
    queries, keyvals, bias, meta = project(
        lengths, chosen[:, 0, :], tokens, w_query, w_key, w_value
    )
    attended = lax.cond(
        meta[2, 0] > 0,
        functools.partial(exchange, LIGHT, 0),
        functools.partial(exchange, FULL, 1),
        bias, meta, queries, keyvals,
    )
    return finish(meta, attended, w_output)


def solution(mesh):
    return jax.shard_map(
        per_device,
        mesh=mesh,
        in_specs=(
            P(None, "kv", None),
            P(None, "tp"),
            P(None, "tp"),
            P(None, "tp"),
            P(None, "tp"),
            P(None, "kv", None),
            P(),
        ),
        out_specs=P(None, "kv", "tp"),
        check_vma=False,
    )
```

```python
import functools

import jax
import jax.numpy as jnp
from jax import lax
from jax.experimental import pallas as pl
from jax.experimental.pallas import tpu as pltpu
from jax.sharding import PartitionSpec as P

SEQS = 8
BLK = 128
SEL = 32
HD = 64
MESH = pl.DeviceIdType.MESH
LOG2E = 1.4426950408889634
NEG = -1e30
GROUPS = ((0, 2), (2, 2), (4, 1), (5, 3))
SKEW = (0, 0, 2, 2)
SIDE = (1, -1, -1, 1)
STRAIGHT = (True, True, True, True)
UPTO = (3, 4, 5, 7, 7, 7, 7, 7)
FULL = ((8, 8, 7, 5, 4, 3, 3, 2), (8, 7, 4, 3))
LIGHT = ((8, 8, 5, 4, 2, 2, 2, 1), (8, 4, 3, 2))


def project_kernel(
    len_ref, chosen_ref, tok_ref, wq_ref, wk_ref, wv_ref,
    q_ref, kv_ref, bias_ref, meta_ref, tok_buf, w_buf, wt_buf, row_buf, sems, w_sems,
):
    block = lax.axis_index("kv")
    first = block * BLK
    weights = (
        pltpu.make_async_copy(wk_ref, wt_buf.at[0:HD], w_sems.at[0]),
        pltpu.make_async_copy(wv_ref, wt_buf.at[HD : 2 * HD], w_sems.at[1]),
        pltpu.make_async_copy(wq_ref, w_buf.at[:, 0:128], w_sems.at[2]),
    )
    for copy in weights:
        copy.start()
    for s in range(SEQS):
        rank = jnp.int32(0)
        for t in range(SEQS):
            if t != s:
                ahead = len_ref[t] > len_ref[s] if t > s else len_ref[t] >= len_ref[s]
                rank = rank + ahead.astype(jnp.int32)
        meta_ref[0, rank] = jnp.int32(s)
        meta_ref[1, rank] = len_ref[s]
    light = jnp.int32(1)
    for row, most in enumerate(LIGHT[0]):
        if most < SEQS:
            light = jnp.where(meta_ref[1, most] > 8 * BLK * row, 0, light)
    for i in range(SEQS):
        meta_ref[2, i] = light

    def fetch(r):
        return pltpu.make_async_copy(tok_ref.at[meta_ref[0, r]], tok_buf.at[r], sems.at[r])

    for r in range(SEQS):
        fetch(r).start()
    for r in range(SEQS):
        row_buf[r : r + 1] = chosen_ref[pl.ds(meta_ref[0, r], 1)]
    picked = row_buf[...]
    for c in range(64):
        listed = jnp.max(jnp.where(picked == c, 0.0, NEG), axis=1, keepdims=True)
        bias_ref[:, c * BLK : (c + 1) * BLK] = jnp.broadcast_to(listed, (SEQS, BLK))
    weights[0].wait()
    weights[1].wait()
    w_buf[:, 128:256] = wt_buf[...].T
    weights[2].wait()
    lane = lax.broadcasted_iota(jnp.int32, (BLK, 128), 1)
    for g in range(SEQS // 2):
        for r in (2 * g, 2 * g + 1):
            fetch(r).wait()
        live = meta_ref[1, 2 * g] > first

        @pl.when(live)
        def _():
            rows = tok_buf[2 * g : 2 * g + 2].reshape(2 * BLK, -1)
            out = jnp.dot(rows, w_buf[...], preferred_element_type=jnp.float32)
            for i in range(2):
                part = out[i * BLK : (i + 1) * BLK]
                q = part[:, 0:128]
                q_ref[2 * g + i, 0:128] = jnp.where(lane < HD, q, 0.0).astype(jnp.bfloat16)
                q_ref[2 * g + i, 128:256] = jnp.where(
                    lane < HD, pltpu.roll(q, HD, 1), 0.0
                ).astype(jnp.bfloat16)
                kv_ref[2 * g + i] = part[:, 128:256].astype(jnp.bfloat16)

        @pl.when(jnp.logical_not(live))
        def _():
            q_ref[2 * g : 2 * g + 2] = jnp.zeros((2, 2 * BLK, 128), jnp.bfloat16)
            kv_ref[2 * g : 2 * g + 2] = jnp.zeros((2, BLK, 128), jnp.bfloat16)


def project(lengths, picked, tokens, w_query, w_key, w_value):
    smem = pl.BlockSpec(memory_space=pltpu.SMEM)
    vmem = pl.BlockSpec(memory_space=pltpu.VMEM)
    hbm = pl.BlockSpec(memory_space=pltpu.HBM)
    return pl.pallas_call(
        project_kernel,
        name="project",
        out_shape=(
            jax.ShapeDtypeStruct((SEQS, 2 * BLK, 128), jnp.bfloat16),
            jax.ShapeDtypeStruct((SEQS, BLK, 128), jnp.bfloat16),
            jax.ShapeDtypeStruct((SEQS, 64 * BLK), jnp.float32),
            jax.ShapeDtypeStruct((3, SEQS), jnp.int32),
        ),
        in_specs=[smem, vmem, hbm, hbm, hbm, hbm],
        out_specs=(vmem, vmem, vmem, smem),
        scratch_shapes=[
            pltpu.VMEM((SEQS, BLK, 2048), jnp.bfloat16),
            pltpu.VMEM((2048, 256), jnp.bfloat16),
            pltpu.VMEM((2 * HD, 2048), jnp.bfloat16),
            pltpu.VMEM((SEQS, SEL), jnp.int32),
            pltpu.SemaphoreType.DMA((SEQS,)),
            pltpu.SemaphoreType.DMA((3,)),
        ],
    )(lengths, picked, tokens, w_query, w_key.T, w_value.T)


def nibble(table):
    packed = sum(v << (4 * i) for i, v in enumerate(table))

    def look(index):
        return (jnp.int32(packed) >> (4 * index)) & 15

    return look


def hop_count(at, row):
    return at - row if at <= UPTO[row] else 8 - at


def exchange_kernel(
    plan, bias_ref, meta_ref, q_ref, kv_ref, att,
    buf, acc, top, own_sem, recv, send, tp_recv, tp_send,
):
    ranks, reach = plan
    ranks_at, upto_at = nibble(ranks), nibble(UPTO)
    hops_max_at = nibble([max(hop_count(at, row) for row in range(at + 1)) for at in range(8)])
    deepest = [
        7 if any(UPTO[row] + 1 < reach[g] for row in range(8)) else reach[g] - 1
        for g in range(len(GROUPS))
    ]
    skew_max_at = nibble([max(SKEW[g] for g in range(len(GROUPS)) if at <= deepest[g]) for at in range(8)])
    block = lax.axis_index("kv")
    member = lax.axis_index("tp")
    z, y = block >> 3, block & 7
    x, core = member >> 1, member & 1
    mine = ranks_at(z)
    first_core = core == 0

    def at_kv(row, col):
        return {"kv": (row & 7) * 8 + (col & 7)}

    def at_tp(chip, which):
        return {"tp": (chip & 3) * 2 + which}

    own = pltpu.make_async_copy(kv_ref, buf.at[:, block], own_sem)
    own.start()
    barrier = pltpu.get_barrier_semaphore()

    def greet(target):
        pl.semaphore_signal(barrier, inc=1, device_id=target, device_id_type=MESH)

    for target in (
        at_kv(z, y + 1), at_kv(z, y - 1),
        at_tp(x + 1, core), at_tp(x - 1, core), at_tp(x + 2, core), at_tp(x, 1 - core),
    ):
        greet(target)
    for step in (1, 2, 6, 7):
        greet(at_kv(z + step, y))

    @pl.when(z == 2)
    def _():
        greet(at_kv(jnp.int32(7), y))

    @pl.when(z == 7)
    def _():
        greet(at_kv(jnp.int32(2), y))

    pl.semaphore_wait(barrier, jnp.where((z == 2) | (z == 7), 11, 10))
    own.wait()

    def link(g, c, sem, target):
        lo, count = GROUPS[g]
        part = buf.at[lo : lo + count, c]
        return pltpu.make_async_remote_copy(
            src_ref=part, dst_ref=part, send_sem=sem, recv_sem=recv.at[g, c],
            device_id=target, device_id_type=MESH,
        )

    def to_long(g, c, row, side):
        link(g, c, send.at[0, g, row], at_kv(z, y + side)).start()

    def to_short(g, c, row, side):
        link(g, c, send.at[1, g, row], at_kv(z, y - side)).start()

    def arrived(g, c):
        link(g, c, send.at[0, 0, 0], at_kv(z, y + 1)).wait_recv()

    def route(row):
        upto = upto_at(row)
        rises = z <= upto
        hops = jnp.where(rises, z - row, 8 - z)
        return upto, rises, hops

    def needs(g, row, upto, rises):
        up = rises & (z < jnp.minimum(upto, reach[g] - 1))
        falls = upto + 1 < reach[g]
        wrap = (z == row) & falls
        down = jnp.logical_not(rises) & (z > upto + 1) & falls
        takes = (rises & (z < reach[g])) | (jnp.logical_not(rises) & falls)
        return takes, up, wrap, down

    def column(g, c, row, up, wrap, down):
        @pl.when(up)
        def _():
            link(g, c, send.at[2, g, row], at_kv(z + 1, y)).start()

        @pl.when(wrap)
        def _():
            link(g, c, send.at[3, g, row], at_kv(jnp.int32(7), y)).start()

        @pl.when(down)
        def _():
            link(g, c, send.at[3, g, row], at_kv(z - 1, y)).start()

    def row_items(u, row, upto, rises):
        for g in range(len(GROUPS)):
            @pl.when(z <= deepest[g])
            def _(g=g):
                step = u - SKEW[g]
                side = SIDE[g]
                takes, up, wrap, down = needs(g, row, upto, rises)
                in_row = row == z

                @pl.when((step >= 0) & (step < 5) & takes)
                def _(g=g, step=step, side=side, up=up, wrap=wrap, down=down, in_row=in_row):
                    c = row * 8 + ((y - side * step) & 7)

                    @pl.when(jnp.logical_not(in_row & (step == 0)))
                    def _():
                        arrived(g, c)

                    @pl.when(in_row & (step < 4))
                    def _():
                        to_long(g, c, row, side)

                    @pl.when(in_row & (step == 0))
                    def _():
                        to_short(g, c, row, side)

                    column(g, c, row, up, wrap, down)

                    @pl.when((step > 0) & (step < 4))
                    def _():
                        c = row * 8 + ((y + side * step) & 7)
                        arrived(g, c)

                        @pl.when(in_row & (step < 3))
                        def _():
                            to_short(g, c, row, side)

                        column(g, c, row, up, wrap, down)

    def column_items(t, row):
        away = z - row
        far = (away + 1) >> 1
        for g in range(len(GROUPS)):
            @pl.when(z <= deepest[g])
            def _(g=g):
                step = t - far - SKEW[g]
                used = z < reach[g]
                side = SIDE[g] * (1 - 2 * (row & 1))

                @pl.when((step == 0) & used)
                def _(g=g, side=side):
                    c = row * 8 + y

                    @pl.when(row != z)
                    def _():
                        arrived(g, c)

                    to_long(g, c, row, side)
                    to_short(g, c, row, side)

                    for ahead in (1, 2):
                        @pl.when(((away & 1) == 0) & (z + ahead < reach[g]))
                        def _(ahead=ahead):
                            link(g, c, send.at[1 + ahead, g, row], at_kv(z + ahead, y)).start()

                @pl.when((step > 0) & (step < 5) & used)
                def _(g=g, step=step, side=side):
                    c = row * 8 + ((y - side * step) & 7)
                    arrived(g, c)

                    @pl.when(step < 4)
                    def _():
                        to_long(g, c, row, side)
                        c2 = row * 8 + ((y + side * step) & 7)
                        arrived(g, c2)

                        @pl.when(step < 3)
                        def _():
                            to_short(g, c2, row, side)

    scale = HD ** (-0.5) * LOG2E
    ones = jnp.ones((8 * BLK, BLK), jnp.bfloat16)
    lane = lax.broadcasted_iota(jnp.int32, (BLK, BLK), 1)
    sub = lax.broadcasted_iota(jnp.int32, (BLK, BLK), 0)

    def scores(r, row, rows, keys):
        raw = lax.dot_general(
            q_ref[r, rows], keys, (((1,), (1,)), ((), ())), preferred_element_type=jnp.float32
        )
        bias = bias_ref[pl.ds(r, 1), pl.ds(pl.multiple_of(row * 8 * BLK, 8 * BLK), 8 * BLK)]
        return raw * scale + bias

    def attend(r, row):
        @pl.when(row == z)
        def _():
            keys = buf[r, pl.ds(row * 8, 8)].reshape(8 * BLK, BLK)
            wide = jnp.concatenate([keys, ones], axis=1)
            for rows in (slice(0, BLK), slice(BLK, 2 * BLK)):
                s = scores(r, row, rows, keys)
                parts = []
                for i in range(8):
                    part = s[:, i * BLK : (i + 1) * BLK]
                    parts.append(jnp.where((lane <= sub) | (y != i), part, NEG))
                s = jnp.concatenate(parts, axis=1)
                best = jnp.max(s, axis=1, keepdims=True)
                p = jnp.exp2(s - best).astype(jnp.bfloat16)
                top[r, rows] = best
                acc[r, rows] = jnp.dot(p, wide, preferred_element_type=jnp.float32)

        @pl.when(row != z)
        def _():
            keys = buf[r, pl.ds(row * 8, 8)].reshape(8 * BLK, BLK)
            wide = jnp.concatenate([keys, ones], axis=1)
            for rows in (slice(0, BLK), slice(BLK, 2 * BLK)):
                s = scores(r, row, rows, keys)
                old = top[r, rows]
                best = jnp.maximum(old, jnp.max(s, axis=1, keepdims=True))
                p = jnp.exp2(s - best).astype(jnp.bfloat16)
                top[r, rows] = best
                acc[r, rows] = acc[r, rows] * jnp.exp2(old - best) + jnp.dot(
                    p, wide, preferred_element_type=jnp.float32
                )

    def settle(r):
        total = acc[r]
        full = total[:, 0:128] / total[:, 128:256]
        both = jnp.where(lane < HD, pltpu.roll(full[0:BLK], HD, 1), full[BLK:])
        both = jnp.where(sub + block * BLK < meta_ref[1, r], both, 0.0)
        att[member, r] = both.astype(jnp.bfloat16)

    def share(g, chip, which, slot, target):
        t = (chip & 3) * 2 + which
        lo, count = GROUPS[g]
        part = att.at[t, lo : lo + count]
        return pltpu.make_async_remote_copy(
            src_ref=part, dst_ref=part, send_sem=tp_send.at[g, slot], recv_sem=tp_recv.at[g, slot],
            device_id=target, device_id_type=MESH,
        )

    right, left, sibling = at_tp(x + 1, core), at_tp(x - 1, core), at_tp(x, 1 - core)

    def share_own(g):
        share(g, x, core, 0, right).start()
        share(g, x, core, 1, left).start()
        share(g, x, core, 2, sibling).start()
        if STRAIGHT[g]:
            share(g, x, core, 3, at_tp(x + 2, core)).start()

    def share_next(g):
        share(g, x - 1, core, 0, right).wait_recv()
        if g % 2 == 0 and not STRAIGHT[g]:
            share(g, x - 1, core, 3, right).start()
        share(g, x - 1, core, 4, sibling).start()
        share(g, x + 1, core, 1, right).wait_recv()
        if g % 2 == 1 and not STRAIGHT[g]:
            share(g, x + 1, core, 3, left).start()
        share(g, x + 1, core, 5, sibling).start()

    def share_far(g):
        share(g, x + 2, core, 3, right).wait_recv()
        share(g, x + 2, core, 6, sibling).start()

    last = len(GROUPS) - 1
    farthest = jnp.where(first_core, hops_max_at(z), (z + 1) >> 1)
    skew_max = skew_max_at(z)

    def delay_of(row):
        return jnp.where(first_core, route(row)[2], (z - row + 1) >> 1)


    def wave(t, carry):
        def comm(i, carry):
            row = jnp.where((z == 2) | (z == 3), i, z - i)
            upto, rises, hops = route(row)
            u = t - hops

            @pl.when(first_core & (u >= 0) & (u <= 4 + skew_max))
            def _():
                row_items(u, row, upto, rises)

            since = t - ((z - row + 1) >> 1)

            @pl.when(jnp.logical_not(first_core) & (since >= 0) & (since <= 4 + skew_max))
            def _():
                column_items(t, row)

            return carry

        lax.fori_loop(0, z + 1, comm, 0)

        def matching(at):
            lo, hi = jnp.int32(8), jnp.int32(0)
            for g, (first, count) in enumerate(GROUPS):
                hit = at == SKEW[g] + 4
                lo = jnp.where(hit, jnp.minimum(lo, first), lo)
                hi = jnp.where(hit, jnp.maximum(hi, first + count), hi)
            return lo, jnp.minimum(hi, mine)

        def compute(i, carry):
            row = z - i
            delay = delay_of(row)
            since = t - delay - 4

            def one(r, carry):
                attend(r, row)
                return carry

            @pl.when((delay < farthest) & (since >= 0) & (since <= skew_max))
            def _():
                lo, hi = matching(t - delay)
                lax.fori_loop(lo, hi, one, 0)

            return carry

        lax.fori_loop(0, z + 1, compute, 0)
        lo, hi = matching(t - farthest)

        def close(r, carry):
            def one(i, carry):
                row = z - i

                @pl.when(delay_of(row) == farthest)
                def _():
                    attend(r, row)

                return carry

            lax.fori_loop(0, z + 1, one, 0)
            settle(r)
            for g, (first, count) in enumerate(GROUPS):
                @pl.when((r >= first) & (r == jnp.minimum(first + count, mine) - 1))
                def _(g=g):
                    share_own(g)
                    if g > 0:
                        share_next(g - 1)
                    if g > 1:
                        share_far(g - 2)

            return carry

        lax.fori_loop(lo, hi, close, 0)
        return carry

    lax.fori_loop(0, farthest + 5 + skew_max, wave, 0)
    for g, (first, count) in enumerate(GROUPS):
        @pl.when((mine > first) & (mine <= first + count))
        def _(g=g):
            share_next(g)
            if g > 0:
                share_far(g - 1)
            share_far(g)

    def sent(direction, g, row, columns):
        lo, count = GROUPS[g]
        part = buf.at[lo : lo + count, 0:columns]
        pltpu.make_async_remote_copy(
            src_ref=part, dst_ref=part, send_sem=send.at[direction, g, row],
            recv_sem=recv.at[0, 0], device_id=right, device_id_type=MESH,
        ).wait_send()

    def drain(row, carry):
        upto, rises, _ = route(row)
        for g in range(len(GROUPS)):
            _, up, wrap, down = needs(g, row, upto, rises)
            ring = (z < reach[g]) & (jnp.logical_not(first_core) | (row == z))

            @pl.when(ring)
            def _(g=g):
                sent(0, g, row, 4)
                sent(1, g, row, 3)

            for direction, used in ((2, up), (3, wrap | down)):
                @pl.when(used & first_core)
                def _(g=g, direction=direction):
                    sent(direction, g, row, 8)

            for ahead in (1, 2):
                straight = jnp.logical_not(first_core) & (((z - row) & 1) == 0)

                @pl.when(straight & (z < reach[g]) & (z + ahead < reach[g]))
                def _(g=g, ahead=ahead):
                    sent(1 + ahead, g, row, 1)

        return carry

    lax.fori_loop(0, z + 1, drain, 0)

    for g in range(len(GROUPS)):
        @pl.when(mine > GROUPS[g][0])
        def _(g=g):
            for chip, slot in ((x, 2), (x - 1, 4), (x + 1, 5), (x + 2, 6)):
                share(g, chip, 1 - core, slot, right).wait_recv()
            for slot in range(7):
                share(g, x, core, slot, right).wait_send()


def exchange(plan, collective, bias, meta, queries, keyvals):
    smem = pl.BlockSpec(memory_space=pltpu.SMEM)
    vmem = pl.BlockSpec(memory_space=pltpu.VMEM)
    return pl.pallas_call(
        functools.partial(exchange_kernel, plan),
        name="exchange",
        out_shape=jax.ShapeDtypeStruct((8, SEQS, BLK, BLK), jnp.bfloat16),
        in_specs=[vmem, smem, vmem, vmem],
        out_specs=vmem,
        scratch_shapes=[
            pltpu.VMEM((SEQS, 64, BLK, BLK), jnp.bfloat16),
            pltpu.VMEM((SEQS, 2 * BLK, 2 * BLK), jnp.float32),
            pltpu.VMEM((SEQS, 2 * BLK, 1), jnp.float32),
            pltpu.SemaphoreType.DMA,
            pltpu.SemaphoreType.DMA((len(GROUPS), 64)),
            pltpu.SemaphoreType.DMA((4, len(GROUPS), 8)),
            pltpu.SemaphoreType.DMA((len(GROUPS), 7)),
            pltpu.SemaphoreType.DMA((len(GROUPS), 7)),
        ],
        compiler_params=pltpu.CompilerParams(
            collective_id=collective, has_side_effects=True, vmem_limit_bytes=48 * 1024 * 1024
        ),
    )(bias, meta, queries, keyvals)


def finish_kernel(meta_ref, att_ref, w_ref, out_ref):
    first = lax.axis_index("kv") * BLK
    for r in range(0, SEQS, 2):
        @pl.when(meta_ref[1, r] > first)
        def _(r=r):
            rows = jnp.concatenate(
                [att_ref[t, r : r + 2].reshape(2 * BLK, BLK) for t in range(8)], axis=1
            )
            mixed = jnp.dot(rows, w_ref[...], preferred_element_type=jnp.float32)
            out_ref[meta_ref[0, r]] = mixed[:BLK].astype(jnp.bfloat16)
            kept = jnp.where(meta_ref[1, r + 1] > first, mixed[BLK:], 0.0)
            out_ref[meta_ref[0, r + 1]] = kept.astype(jnp.bfloat16)

        @pl.when(meta_ref[1, r] <= first)
        def _(r=r):
            for i in (r, r + 1):
                out_ref[meta_ref[0, i]] = jnp.zeros((BLK, 256), jnp.bfloat16)


def finish(meta, attended, w_output):
    vmem = pl.BlockSpec(memory_space=pltpu.VMEM)
    return pl.pallas_call(
        finish_kernel,
        name="finish",
        out_shape=jax.ShapeDtypeStruct((SEQS, BLK, 256), jnp.bfloat16),
        in_specs=[pl.BlockSpec(memory_space=pltpu.SMEM), vmem, vmem],
        out_specs=vmem,
        compiler_params=pltpu.CompilerParams(vmem_limit_bytes=16 * 1024 * 1024),
    )(meta, attended, w_output)


def per_device(tokens, w_query, w_key, w_value, w_output, chosen, lengths):
    queries, keyvals, bias, meta = project(
        lengths, chosen[:, 0, :], tokens, w_query, w_key, w_value
    )
    attended = lax.cond(
        meta[2, 0] > 0,
        functools.partial(exchange, LIGHT, 0),
        functools.partial(exchange, FULL, 1),
        bias, meta, queries, keyvals,
    )
    return finish(meta, attended, w_output)


def solution(mesh):
    return jax.shard_map(
        per_device,
        mesh=mesh,
        in_specs=(
            P(None, "kv", None),
            P(None, "tp"),
            P(None, "tp"),
            P(None, "tp"),
            P(None, "tp"),
            P(None, "kv", None),
            P(),
        ),
        out_specs=P(None, "kv", "tp"),
        check_vma=False,
    )
```
